32 devices in a mesh: ep: 8 (over z, core), tp: 4 (over y, x).
Axes of the slice: x: 2, y: 2, z: 4, core: 2. Of those that a mesh axis runs over, the one named last changes fastest.
Arguments:
- tokens: bfloat16 [512, 4096], P('ep', 'tp'), may hold values from -600 to 600
- in_gain: float32 [4096], P('tp'), may hold values from 0.1 to 1.9
- out_gain: float32 [4096], P('tp'), may hold values from 0.1 to 1.9
- routes: int32 [512, 4], replicated, may hold values from 0 to 31, as said below
- route_weights: float32 [512, 4], replicated, may hold values from 0.05 to 1
- w_gate: bfloat16 [32, 4096, 1024], P('ep', 'tp'), may hold values from -0.09375 to 0.09375
- w_up: bfloat16 [32, 4096, 1024], P('ep', 'tp'), may hold values from -0.09375 to 0.09375
- w_down: bfloat16 [32, 1024, 4096], P('ep', None, 'tp'), may hold values from -0.375 to 0.375
Outputs:
- result: bfloat16 [512, 4096], P('ep', 'tp')
The draws below stay inside these ranges and needn't reach their ends.
Inputs may be any that keep to these rules, and one draw needn't show every extreme that they name: `routes`: each row names 4 different experts, all in one group of 8 consecutive numbers. In the rows of one index of ep (aligned blocks of 64 rows) no expert is named by more than 16 rows, and some expert by exactly 16.
All inputs are finite; a program needn't handle non-finite values.
Results may differ from the reference program's by a relative error of at most 0.025.
Values may be sent and summed in bfloat16 or wider, within the bound.
A program may use at most 64 MiB of HBM per device.

```python
import math
import jax
import jax.numpy as jnp
from jax import lax

D = 4096
FF = 1024
EXP_DEV = 4
GROUP_SIZE = 8
TOP = 4
TOK_DEV = 64
SPECIALIST_COUNT = 32
GROUPS = 4
TOKENS = 512
CAP = 16
N_EP = 8
N_TP = 4


def column_scale(key):
    columns = jnp.arange(D, dtype=jnp.float32) / D
    return jnp.exp(math.log(3.0) * columns + math.log(2.0) * jax.random.uniform(key, (D,), jnp.float32))


def draw_tokens(key, part):
    key_base, key_rows, key_cols = jax.random.split(jax.random.fold_in(key, 3), 3)
    base = jnp.clip(jax.random.normal(key_base, (TOKENS, D), jnp.float32), -6.0, 6.0)
    row_scale = jnp.exp(math.log(10.0) * jax.random.uniform(key_rows, (TOKENS, 1), jnp.float32))
    return (base * column_scale(key_cols) * row_scale).astype(jnp.bfloat16)


def draw_w_down(key, part):
    key_base, key_cols = jax.random.split(jax.random.fold_in(key, 5))
    base = jnp.clip(jax.random.normal(key_base, (SPECIALIST_COUNT, FF, D), jnp.float32), -6.0, 6.0)
    return (base * column_scale(key_cols) * FF ** (-0.5) / 3.0).astype(jnp.bfloat16)


def draw_routes(key, part):
    blocks = TOKENS // TOK_DEV
    key_rank, key_rows = jax.random.split(jax.random.fold_in(key, 7))
    ranking = jax.random.permutation(key_rank, SPECIALIST_COUNT).astype(jnp.int32)
    preferred_specialists = 12 * SPECIALIST_COUNT // (ranking + 1)
    numbers = jnp.arange(SPECIALIST_COUNT, dtype=jnp.int32)
    specialist_holders = numbers // EXP_DEV
    inside = jnp.arange(GROUP_SIZE, dtype=jnp.int32)
    group_ids = jnp.arange(GROUPS, dtype=jnp.int32)
    noise = jax.random.randint(key_rows, (blocks, TOK_DEV, SPECIALIST_COUNT), 0, 4 * SPECIALIST_COUNT, dtype=jnp.int32)

    def one_block(block, noise_rows):

        def step(counts, inputs):
            present_sequence_entry, jitter_for_entry = inputs
            destination_specialist = jnp.where(present_sequence_entry == 0, (block + blocks - 1) % blocks, (block + blocks // 2) % blocks)
            logit_offset = jnp.where((present_sequence_entry < 2) & (specialist_holders == destination_specialist), 64 * SPECIALIST_COUNT, 0).astype(jnp.int32)
            gating_logit = preferred_specialists + jitter_for_entry + logit_offset
            is_free = counts < CAP
            masked = jnp.where(is_free, gating_logit, -1).reshape(GROUPS, GROUP_SIZE)
            enough = jnp.sum(is_free.reshape(GROUPS, GROUP_SIZE).astype(jnp.int32), axis=1) >= TOP
            group_key = jnp.where(enough, jnp.max(masked, axis=1), -2) * GROUPS + group_ids
            chosen = jnp.argmax(group_key).astype(jnp.int32)
            within = lax.dynamic_index_in_dim(masked, chosen, 0, keepdims=False)
            best = lax.top_k(within * GROUP_SIZE + inside, TOP)[1].astype(jnp.int32)
            picked = chosen * GROUP_SIZE + best
            counts = counts + jnp.sum((picked[:, None] == numbers[None, :]).astype(jnp.int32), axis=0)
            return (counts, picked)
        row_ids = jnp.arange(TOK_DEV, dtype=jnp.int32)
        return lax.scan(step, jnp.zeros((SPECIALIST_COUNT,), jnp.int32), (row_ids, noise_rows))[1]
    picked_all = jax.vmap(one_block)(jnp.arange(blocks, dtype=jnp.int32), noise)
    return picked_all.reshape(TOKENS, TOP).astype(jnp.int32)


def block_scale(key, dims, cuts, smallest, top_value):
    factor_of, own = 1.0, jax.random.fold_in(key, 6)
    for dim, blocks in cuts:
        draws = jnp.exp(jax.random.uniform(jax.random.fold_in(own, dim), (blocks,), jnp.float32, smallest / len(cuts), top_value / len(cuts)))
        factor_of = factor_of * jnp.repeat(draws, dims[dim] // blocks).reshape([-1 if axis == dim else 1 for axis in range(len(dims))])
    return factor_of


def normal_values(stream_key, shape, width, limit, shards=(), kind=jnp.bfloat16):
    drawn = width * jax.random.normal(stream_key, shape, jnp.float32)
    if shards:
        drawn = drawn * block_scale(stream_key, shape, shards, -0.22, 0.18)
    return jnp.clip(drawn, -limit, limit).astype(kind)


def setup_inputs(seed: int = 0) -> dict:
    arg_keys = jax.random.split(jax.random.key(seed), 9)
    tokens = draw_tokens(jax.random.fold_in(arg_keys[8], 71), 0)
    in_gain = jnp.clip(1.0 + 0.18 * jax.random.normal(arg_keys[1], (D,), jnp.float32), 0.1, 1.9)
    out_gain = jnp.clip(1.0 + 0.18 * jax.random.normal(arg_keys[2], (D,), jnp.float32), 0.1, 1.9)
    routes = draw_routes(jax.random.fold_in(arg_keys[8], 71), 0)
    route_weights = jnp.clip(jax.random.uniform(arg_keys[4], (TOKENS, TOP), jnp.float32, 0.05, 1.0), 0.05, 1.0)
    w_gate = normal_values(arg_keys[5], (SPECIALIST_COUNT, D, FF), D ** -0.5, 0.09375, ((0, 8), (1, 4)))
    w_up = normal_values(arg_keys[6], (SPECIALIST_COUNT, D, FF), D ** -0.5, 0.09375, ((0, 8), (1, 4)))
    w_down = draw_w_down(jax.random.fold_in(arg_keys[8], 71), 0)
    return dict(tokens=tokens, in_gain=in_gain, out_gain=out_gain, routes=routes, route_weights=route_weights, w_gate=w_gate, w_up=w_up, w_down=w_down)


EPS = 1e-06

def reference(tokens, in_gain, out_gain, routes, route_weights, w_gate, w_up, w_down):
    values = tokens.astype(jnp.float32)
    normed = (values * lax.rsqrt(lax.optimization_barrier(jnp.mean(values * values, axis=1, keepdims=True)) + EPS) * in_gain).astype(jnp.bfloat16)
    local_width = D // N_TP
    slot_limit = N_EP * CAP

    def block_sum(slot_rows, weights):
        stacked = weights.astype(jnp.float32).reshape(N_TP, local_width, FF)
        parts = jnp.einsum('rjd,jdf->jrf', slot_rows, stacked).astype(jnp.bfloat16)
        parts = lax.optimization_barrier(parts)
        return lax.optimization_barrier(jnp.sum(parts.astype(jnp.float32), axis=0))

    def one_expert(combined, expert):
        matches = routes == expert
        weight = lax.optimization_barrier(jnp.sum(jnp.where(matches, route_weights, 0.0), axis=1))
        chosen = jnp.any(matches, axis=1)
        picked = jnp.nonzero(chosen, size=slot_limit, fill_value=0)[0].astype(jnp.int32)
        is_live = jnp.arange(slot_limit, dtype=jnp.int32) < jnp.sum(chosen.astype(jnp.int32))
        slot_rows = normed[picked].astype(jnp.float32).reshape(slot_limit, N_TP, local_width)
        gate_sum = block_sum(slot_rows, w_gate[expert])
        up_sum = block_sum(slot_rows, w_up[expert])
        active = (jax.nn.silu(gate_sum) * up_sum).astype(jnp.bfloat16)
        results = jnp.dot(active, w_down[expert], preferred_element_type=jnp.float32).astype(jnp.bfloat16)
        scale = jnp.where(is_live, weight[picked], 0.0)
        combined = combined.at[picked].add(scale[:, None] * results.astype(jnp.float32))
        return (combined, None)
    start = jnp.zeros((TOKENS, D), jnp.float32)
    combined, unused = lax.scan(one_expert, start, jnp.arange(SPECIALIST_COUNT, dtype=jnp.int32))
    squares = lax.optimization_barrier(jnp.mean(combined * combined, axis=1, keepdims=True))
    return (combined * lax.rsqrt(squares + EPS) * out_gain).astype(jnp.bfloat16)
```

```python
import functools

import jax
import jax.numpy as jnp
from jax import lax
from jax.experimental import pallas as pl
from jax.experimental.pallas import tpu as pltpu
from jax.sharding import PartitionSpec as P

D = 4096
GROUP = 8

EPS = 1e-06
MESH = pl.DeviceIdType.MESH
F32, BF16 = jnp.float32, jnp.bfloat16


def iota(shape, dim):
    return lax.broadcasted_iota(jnp.int32, shape, dim)


def tdot(a, b):
    return lax.dot_general(a, b, (((0,), (0,)), ((), ())), preferred_element_type=F32)


def kernel(
    cfg,
    tokens_ref,
    in_gain_ref,
    out_gain_ref,
    routes_ref,
    weights_ref,
    wg_hbm,
    wu_hbm,
    wd_hbm,
    out_ref,
    wg,
    wu,
    wd,
    pick,
    slot_w,
    own_pick,
    ss_out,
    ss_in,
    send_rows,
    compact,
    part,
    s1_in,
    keep,
    s2_out,
    s2_in,
    act,
    comb,
    x_out,
    x_in,
    r_out,
    r_in,
    w_sem,
    ss_send,
    ss_recv,
    d_send,
    f_send,
    d_recv,
    s1_send,
    s1_recv,
    s2_send,
    s2_recv,
    g1_send,
    g1_recv,
    g2_send,
    g2_recv,
    x_send,
    x_recv,
    r_send,
    r_recv,
):
    n_ep, n_z, tok, n_exp, cap, width, ff, top = cfg
    rows_z = cap * GROUP // top
    tok_all = n_ep * tok
    me = lax.axis_index("ep")
    tp = lax.axis_index("tp")
    z, core = me // 2, lax.rem(me, 2)
    other = 1 - core
    y, x = tp // 2, lax.rem(tp, 2)
    x_tp = 2 * y + (1 - x)
    y_tp = 2 * (1 - y) + x
    xy_tp = 2 * (1 - y) + (1 - x)
    partner = 2 * z + other
    peers = (x_tp, y_tp, xy_tp)

    for j in range(n_exp):
        pltpu.make_async_copy(wg_hbm.at[j], wg.at[j], w_sem.at[0, j]).start()
        pltpu.make_async_copy(wu_hbm.at[j], wu.at[j], w_sem.at[1, j]).start()
    for j in range(n_exp):
        pltpu.make_async_copy(wd_hbm.at[j], wd.at[j], w_sem.at[2, j]).start()

    def far_ep(dz):
        return 2 * lax.rem(z + dz, n_z) + core

    barrier = pltpu.get_barrier_semaphore()
    for peer in peers:
        pl.semaphore_signal(barrier, inc=1, device_id={"tp": peer}, device_id_type=MESH)
    pl.semaphore_signal(barrier, inc=1, device_id={"ep": partner}, device_id_type=MESH)
    for dz in range(1, n_z):
        pl.semaphore_signal(barrier, inc=1, device_id={"ep": far_ep(dz)}, device_id_type=MESH)

    def remote(src, dst, send, recv, axis, dev):
        return pltpu.make_async_remote_copy(
            src_ref=src,
            dst_ref=dst,
            send_sem=send,
            recv_sem=recv,
            device_id={axis: dev},
            device_id_type=MESH,
        )

    def square_copy(which, k):
        return remote(
            ss_out.at[which],
            ss_in.at[which, k],
            ss_send.at[which, k],
            ss_recv.at[which, k],
            "tp",
            peers[k],
        )

    values = tokens_ref[...].astype(F32)
    square = jnp.sum(values * values, axis=1, keepdims=True)
    ss_out[0] = jnp.broadcast_to(square, (tok, 128))

    lane = iota((tok, 128), 1)
    own_routes = routes_ref[pl.ds(me * tok, tok), :]
    group = own_routes[:, 0:1] // GROUP
    in_group = (lane == group).astype(F32)
    before = (iota((tok, tok), 1) < iota((tok, tok), 0)).astype(BF16)
    ranks = jnp.dot(before, in_group.astype(BF16), preferred_element_type=F32)
    rank = jnp.sum(ranks * in_group, axis=1, keepdims=True).astype(jnp.int32)
    own_lane = iota((tok, n_z * rows_z), 1)
    own_pick[...] = (own_lane == group * rows_z + rank).astype(BF16)

    pl.semaphore_wait(barrier, 4 + n_z - 1)
    for k in range(3):
        square_copy(0, k).start()

    routes = routes_ref[...]
    lane = iota((tok_all, 128), 1)
    row_block = iota((tok_all, 128), 0) // tok
    first = me * n_exp
    hits = jnp.where((lane == n_exp) & (routes[:, 0:1] // GROUP == z), 1.0, 0.0)
    wt = jnp.zeros((tok_all, 128), F32)
    for k in range(top):
        match = (routes[:, k : k + 1] == first + lane) & (lane < n_exp)
        hits = hits + jnp.where(match, 1.0, 0.0)
        wt = wt + jnp.where(match, weights_ref[:, k : k + 1], 0.0)
    t_row, t_col = iota((tok_all, tok_all), 0), iota((tok_all, tok_all), 1)
    before = ((t_col < t_row) & (t_col // tok == t_row // tok)).astype(BF16)
    ranks = jnp.dot(before, hits.astype(BF16), preferred_element_type=F32)
    rank = jnp.where(hits > 0.0, ranks, -1.0).astype(jnp.int32)
    wide = iota((tok_all, n_ep * rows_z), 1)
    wide_block = iota((tok_all, n_ep * rows_z), 0) // tok
    group_rows = (
        (rank[:, n_exp : n_exp + 1] == wide % rows_z) & (wide // rows_z == wide_block)
    ).astype(BF16)
    w_hi = wt.astype(BF16)
    w_mid = (wt - w_hi.astype(F32)).astype(BF16)
    w_lo = (wt - w_hi.astype(F32) - w_mid.astype(F32)).astype(BF16)
    slots = n_ep * cap
    for j in range(n_exp):
        slot = (
            (rank[:, j : j + 1] == lane % cap) & (lane // cap == row_block)
        ).astype(BF16)
        pick[j] = tdot(slot, group_rows).astype(BF16)
        weight = tdot(slot, w_hi) + tdot(slot, w_mid) + tdot(slot, w_lo)
        weight = jnp.sum(jnp.where(iota((slots, 128), 1) == j, weight, 0.0), axis=1, keepdims=True)
        slot_w[j] = jnp.broadcast_to(weight, (slots, 128)).reshape(n_ep, cap, 128)

    for k in range(3):
        square_copy(0, k).wait_recv()
    square = ss_out[0] + ss_in[0, 0] + ss_in[0, 1] + ss_in[0, 2]
    scale = lax.rsqrt(square[:, 0:1] / D + EPS)
    normed = (values * scale * in_gain_ref[...]).astype(BF16)
    send_rows[...] = tdot(own_pick[...], normed).astype(BF16).reshape(n_z, rows_z, width)

    def dispatch(dz, src_block, far):
        return remote(
            send_rows.at[lax.rem(z + dz, n_z)],
            compact.at[src_block],
            d_send.at[dz - 1],
            d_recv.at[src_block],
            "ep",
            far,
        )

    def forward(k, block):
        return remote(
            compact.at[block], compact.at[block], f_send.at[k], d_recv.at[block], "ep", partner
        )

    for dz in range(1, n_z):
        dispatch(dz, me, far_ep(dz)).start()
    compact[me] = send_rows[z]
    own_forward = remote(
        send_rows.at[z], compact.at[me], f_send.at[0], d_recv.at[me], "ep", partner
    )
    own_forward.start()
    for dz in range(1, n_z):
        block = 2 * lax.rem(z - dz + n_z, n_z) + core
        dispatch(dz, block, far_ep(dz)).wait_recv()
        forward(dz, block).start()
    for dz in range(n_z):
        block = 2 * lax.rem(z - dz + n_z, n_z) + other
        forward(0, block).wait_recv()

    half = n_ep // 2

    def side(h):
        return (x_tp, y_tp, x, y) if h == 0 else (y_tp, x_tp, y, x)

    def s1(j, h):
        near, _, a, _ = side(h)
        return remote(
            part.at[j, pl.ds(h * half + 2 * (1 - a), 2)],
            s1_in.at[j, h],
            s1_send.at[j, h],
            s1_recv.at[j, h],
            "tp",
            near,
        )

    def s2(j, h):
        return remote(
            s2_out.at[j, h], s2_in.at[j, h], s2_send.at[j, h], s2_recv.at[j, h], "tp", side(h)[1]
        )

    def g1(j, h):
        _, near, a, b = side(h)
        piece = act.at[j, h * half + 2 * a + b]
        return remote(piece, piece, g1_send.at[j, h], g1_recv.at[j, h], "tp", near)

    def g2(j, h):
        near, _, a, _ = side(h)
        piece = act.at[j, pl.ds(h * half + 2 * a, 2)]
        return remote(piece, piece, g2_send.at[j, h], g2_recv.at[j, h], "tp", near)

    def w_wait(k, j, hbm, vmem):
        pltpu.make_async_copy(hbm.at[j], vmem.at[j], w_sem.at[k, j]).wait()

    @pl.loop(0, n_exp)
    def _(j):
        rows = jnp.dot(
            pick[j], compact[...].reshape(n_ep * rows_z, width), preferred_element_type=F32
        ).astype(BF16)
        w_wait(0, j, wg_hbm, wg)
        part[j, :, :, 0:ff] = (
            jnp.dot(rows, wg[j], preferred_element_type=F32).astype(BF16).reshape(n_ep, cap, ff)
        )
        w_wait(1, j, wu_hbm, wu)
        part[j, :, :, ff : 2 * ff] = (
            jnp.dot(rows, wu[j], preferred_element_type=F32).astype(BF16).reshape(n_ep, cap, ff)
        )
        for h in range(2):
            s1(j, h).start()

    @pl.loop(0, n_exp)
    def _(j):
        for h in range(2):
            _, _, a, b = side(h)
            s1(j, h).wait_recv()
            mine = h * half + 2 * a
            s2_out[j, h] = (
                part[j, mine + 1 - b].astype(F32) + s1_in[j, h, 1 - b].astype(F32)
            ).astype(BF16)
            s2(j, h).start()
            keep[j, h] = part[j, mine + b].astype(F32) + s1_in[j, h, b].astype(F32)

    @pl.loop(0, n_exp)
    def _(j):
        for h in range(2):
            _, _, a, b = side(h)
            s2(j, h).wait_recv()
            piece = h * half + 2 * a + b
            total = keep[j, h] + s2_in[j, h].astype(F32)
            gate, up = total[:, 0:ff], total[:, ff : 2 * ff]
            act[j, piece] = (
                gate / (1.0 + jnp.exp(-gate)) * up * slot_w[j, piece][:, 0:1]
            ).astype(BF16)
            g1(j, h).start()

    @pl.loop(0, n_exp)
    def _(j):
        for h in range(2):
            g1(j, h).wait_recv()
            g2(j, h).start()

    comb[...] = jnp.zeros_like(comb)

    @pl.loop(0, n_exp)
    def _(j):
        w_wait(2, j, wd_hbm, wd)
        for h in range(2):
            g2(j, h).wait_recv()
        result = jnp.dot(
            act[j].reshape(slots, ff), wd[j], preferred_element_type=F32
        ).astype(BF16)
        comb[...] += tdot(pick[j], result).reshape(n_z, 2, rows_z, width)

    def swap(k):
        return remote(x_out.at[k], x_in.at[k], x_send.at[k], x_recv.at[k], "ep", partner)

    def home(dz, far):
        return remote(
            r_out.at[dz], r_in.at[z], r_send.at[dz - 1], r_recv.at[z], "ep", far
        )

    def home_in(dz):
        block = lax.rem(z - dz + n_z, n_z)
        return remote(
            r_out.at[dz], r_in.at[block], r_send.at[dz - 1], r_recv.at[block], "ep", far_ep(dz)
        )

    for dz in range(1, n_z + 1):
        k = dz % n_z
        x_out[k] = comb[lax.rem(z + dz, n_z), other].astype(BF16)
        swap(k).start()
    for dz in range(1, n_z + 1):
        k = dz % n_z
        mine = comb[lax.rem(z + dz, n_z), core]
        swap(k).wait_recv()
        total = (mine + x_in[k].astype(F32)).astype(BF16)
        if k:
            r_out[k] = total
            home(k, far_ep(k)).start()
        else:
            r_in[z] = total
    for dz in range(1, n_z):
        home_in(dz).wait_recv()

    combined = jnp.dot(
        own_pick[...], r_in[...].reshape(n_z * rows_z, width), preferred_element_type=F32
    )
    square = jnp.sum(combined * combined, axis=1, keepdims=True)
    ss_out[1] = jnp.broadcast_to(square, (tok, 128))
    for k in range(3):
        square_copy(1, k).start()
    for k in range(3):
        square_copy(1, k).wait_recv()
    square = ss_out[1] + ss_in[1, 0] + ss_in[1, 1] + ss_in[1, 2]
    scale = lax.rsqrt(square[:, 0:1] / D + EPS)
    out_ref[...] = (combined * scale * out_gain_ref[...]).astype(BF16)

    for k in range(3):
        square_copy(0, k).wait_send()
        square_copy(1, k).wait_send()
    own_forward.wait_send()
    for dz in range(1, n_z):
        dispatch(dz, me, far_ep(dz)).wait_send()
        forward(dz, me).wait_send()
        home(dz, far_ep(dz)).wait_send()
    for k in range(n_z):
        swap(k).wait_send()

    @pl.loop(0, n_exp)
    def _(j):
        for h in range(2):
            s1(j, h).wait_send()
            s2(j, h).wait_send()
            g1(j, h).wait_send()
            g2(j, h).wait_send()


def fused(mesh, tokens, in_gain, out_gain, routes, route_weights, w_gate, w_up, w_down):
    tok, width = tokens.shape
    top = routes.shape[1]
    n_exp, _, ff = w_gate.shape
    n_ep = mesh.shape["ep"]
    n_z = n_ep // 2
    cap = max(2, 2 * tok * top // (n_exp * n_ep))
    rows_z = cap * GROUP // top
    cfg = (n_ep, n_z, tok, n_exp, cap, width, ff, top)
    vmem = pl.BlockSpec(memory_space=pltpu.VMEM)
    hbm = pl.BlockSpec(memory_space=pl.ANY)
    dma = pltpu.SemaphoreType.DMA
    return pl.pallas_call(
        functools.partial(kernel, cfg),
        out_shape=jax.ShapeDtypeStruct((tok, width), BF16),
        in_specs=[vmem] * 5 + [hbm] * 3,
        out_specs=vmem,
        scratch_shapes=[
            pltpu.VMEM(w_gate.shape, BF16),
            pltpu.VMEM(w_up.shape, BF16),
            pltpu.VMEM(w_down.shape, BF16),
            pltpu.VMEM((n_exp, n_ep * cap, n_ep * rows_z), BF16),
            pltpu.VMEM((n_exp, n_ep, cap, 128), F32),
            pltpu.VMEM((tok, n_z * rows_z), BF16),
            pltpu.VMEM((2, tok, 128), F32),
            pltpu.VMEM((2, 3, tok, 128), F32),
            pltpu.VMEM((n_z, rows_z, width), BF16),
            pltpu.VMEM((n_ep, rows_z, width), BF16),
            pltpu.VMEM((n_exp, n_ep, cap, 2 * ff), BF16),
            pltpu.VMEM((n_exp, 2, 2, cap, 2 * ff), BF16),
            pltpu.VMEM((n_exp, 2, cap, 2 * ff), F32),
            pltpu.VMEM((n_exp, 2, cap, 2 * ff), BF16),
            pltpu.VMEM((n_exp, 2, cap, 2 * ff), BF16),
            pltpu.VMEM((n_exp, n_ep, cap, ff), BF16),
            pltpu.VMEM((n_z, 2, rows_z, width), F32),
            pltpu.VMEM((n_z, rows_z, width), BF16),
            pltpu.VMEM((n_z, rows_z, width), BF16),
            pltpu.VMEM((n_z, rows_z, width), BF16),
            pltpu.VMEM((n_z, rows_z, width), BF16),
            dma((3, n_exp)),
            dma((2, 3)),
            dma((2, 3)),
            dma((n_z - 1,)),
            dma((n_z,)),
            dma((n_ep,)),
        ]
        + [dma((n_exp, 2))] * 8
        + [dma((n_z,)), dma((n_z,)), dma((n_z - 1,)), dma((n_z,))],
        compiler_params=pltpu.CompilerParams(
            collective_id=0, has_side_effects=True, vmem_limit_bytes=60 * 2**20
        ),
    )(
        tokens,
        in_gain.reshape(1, width),
        out_gain.reshape(1, width),
        routes,
        route_weights,
        w_gate,
        w_up,
        w_down,
    )


def run_experts(slot_rows, w_gate, w_up, w_down):
    gate_part = jnp.einsum(
        "secd,edf->secf", slot_rows, w_gate, preferred_element_type=jnp.float32
    ).astype(jnp.bfloat16)
    up_part = jnp.einsum(
        "secd,edf->secf", slot_rows, w_up, preferred_element_type=jnp.float32
    ).astype(jnp.bfloat16)
    gate_sum, up_sum = (
        lax.psum(gate_part, "tp").astype(jnp.float32),
        lax.psum(up_part, "tp").astype(jnp.float32),
    )
    active = (jax.nn.silu(gate_sum) * up_sum).astype(jnp.bfloat16)
    return jnp.einsum("secf,efd->secd", active, w_down, preferred_element_type=jnp.float32).astype(
        jnp.bfloat16
    )


def on_device(tokens, in_gain, out_gain, routes, route_weights, w_gate, w_up, w_down):
    tok_rows, local_width = tokens.shape
    top_count = routes.shape[1]
    local_experts = w_gate.shape[0]
    groups_ep = lax.axis_size("ep")
    experts = local_experts * groups_ep
    capacity = max(2, 2 * tok_rows * top_count // experts)
    values = tokens.astype(jnp.float32)
    sum_squares = lax.psum(jnp.sum(values * values, axis=1), "tp")
    normed = (values * lax.rsqrt(sum_squares / D + EPS)[:, None] * in_gain).astype(jnp.bfloat16)
    row_start = lax.axis_index("ep") * tok_rows
    my_routes = lax.dynamic_slice_in_dim(routes, row_start, tok_rows, 0)
    my_weights = lax.dynamic_slice_in_dim(route_weights, row_start, tok_rows, 0)
    flat_ids = my_routes.reshape(-1)
    matches = (flat_ids[:, None] == jnp.arange(experts, dtype=jnp.int32)[None, :]).astype(jnp.int32)
    slot_rank = jnp.sum((jnp.cumsum(matches, axis=0) - matches) * matches, axis=1)
    position = flat_ids * capacity + slot_rank
    dispatch_table = jnp.any(
        position.reshape(tok_rows, top_count, 1)
        == jnp.arange(experts * capacity, dtype=jnp.int32)[None, None, :],
        axis=1,
    )
    outgoing = jnp.einsum(
        "ts,td->sd", dispatch_table.astype(jnp.bfloat16), normed, preferred_element_type=jnp.float32
    ).astype(jnp.bfloat16)
    outgoing = outgoing.reshape(groups_ep, local_experts, capacity, local_width)
    answers = run_experts(
        lax.all_to_all(outgoing, "ep", split_axis=0, concat_axis=0, tiled=True),
        w_gate,
        w_up,
        w_down,
    )
    returned = lax.all_to_all(answers, "ep", split_axis=0, concat_axis=0, tiled=True)
    flat_out = returned.reshape(experts * capacity, local_width)
    picked = flat_out[position].reshape(tok_rows, top_count, local_width)
    combined = jnp.sum(my_weights[:, :, None] * picked.astype(jnp.float32), axis=1)
    out_squares = lax.psum(jnp.sum(combined * combined, axis=1), "tp")
    return (combined * lax.rsqrt(out_squares / D + EPS)[:, None] * out_gain).astype(jnp.bfloat16)


def solution(mesh):
    placed = (
        P("ep", "tp"),
        P("tp"),
        P("tp"),
        P(),
        P(),
        P("ep", "tp", None),
        P("ep", "tp", None),
        P("ep", None, "tp"),
    )
    body = on_device
    if mesh.shape["tp"] == 4 and mesh.shape["ep"] == 8:
        body = functools.partial(fused, mesh)
    return jax.shard_map(
        body, mesh=mesh, in_specs=placed, out_specs=P("ep", "tp"), check_vma=False
    )
```

```python
import functools

import jax
import jax.numpy as jnp
from jax import lax
from jax.experimental import pallas as pl
from jax.experimental.pallas import tpu as pltpu
from jax.sharding import PartitionSpec as P

D = 4096
GROUP = 8

EPS = 1e-06
MESH = pl.DeviceIdType.MESH
F32, BF16 = jnp.float32, jnp.bfloat16


def iota(shape, dim):
    return lax.broadcasted_iota(jnp.int32, shape, dim)


def tdot(a, b):
    return lax.dot_general(a, b, (((0,), (0,)), ((), ())), preferred_element_type=F32)


def kernel(cfg, *refs):
    n_z, tok, n_exp, cap, width, ff, top, chunks = cfg
    it = iter(refs)
    tokens_ref, in_gain_ref, out_gain_ref, routes_ref, weights_ref = [next(it) for _ in range(5)]
    wg_hbm, wu_hbm, wd_hbm, out_ref, wg, wu, wd = [next(it) for _ in range(7)]
    route_t, weight_t, pick, slot_w, own_pick = [next(it) for _ in range(5)]
    ss_out, ss_in, send_rows, compact, x_out, x_in, r_out, r_in = [next(it) for _ in range(8)]
    bufs = [[next(it) for _ in range(9)] for _ in chunks]
    w_sem, ss_send, ss_recv, d_send, f_send, d_recv, f_recv = [next(it) for _ in range(7)]
    x_send, x_recv, r_send, r_recv = [next(it) for _ in range(4)]
    sems = [[next(it) for _ in range(8)] for _ in chunks]

    rows_z = cap * GROUP // top
    pair = 2 * tok
    piece_cols = ff // 8
    me = lax.axis_index("ep")
    tp = lax.axis_index("tp")
    z, core = me // 2, lax.rem(me, 2)
    other = 1 - core
    y, x = tp // 2, lax.rem(tp, 2)
    x_tp = 2 * y + (1 - x)
    y_tp = 2 * (1 - y) + x
    xy_tp = 2 * (1 - y) + (1 - x)
    partner = 2 * z + other
    peers = (x_tp, y_tp, xy_tp)
    chips = (z, z + 1 - 2 * lax.rem(z, 2), lax.rem(z + 2, n_z), n_z - 1 - z)
    far_order = [d for chunk in chunks for d in chunk if d]

    for j in range(n_exp):
        pltpu.make_async_copy(wg_hbm.at[j], wg.at[j], w_sem.at[0, j]).start()
        pltpu.make_async_copy(wu_hbm.at[j], wu.at[j], w_sem.at[1, j]).start()
    for j in range(n_exp):
        pltpu.make_async_copy(wd_hbm.at[j], wd.at[j], w_sem.at[2, j]).start()

    def far_ep(d):
        return 2 * chips[d] + core

    barrier = pltpu.get_barrier_semaphore()
    for peer in peers:
        pl.semaphore_signal(barrier, inc=1, device_id={"tp": peer}, device_id_type=MESH)
    pl.semaphore_signal(barrier, inc=1, device_id={"ep": partner}, device_id_type=MESH)
    for d in far_order:
        pl.semaphore_signal(barrier, inc=1, device_id={"ep": far_ep(d)}, device_id_type=MESH)

    def remote(src, dst, send, recv, axis, dev):
        return pltpu.make_async_remote_copy(
            src_ref=src,
            dst_ref=dst,
            send_sem=send,
            recv_sem=recv,
            device_id={axis: dev},
            device_id_type=MESH,
        )

    def square_copy(which, k):
        return remote(
            ss_out.at[which],
            ss_in.at[which, k],
            ss_send.at[which, k],
            ss_recv.at[which, k],
            "tp",
            peers[k],
        )

    values = tokens_ref[...].astype(F32)
    square = jnp.sum(values * values, axis=1, keepdims=True)
    ss_out[0] = jnp.broadcast_to(square, (tok, 128))
    pl.semaphore_wait(barrier, 4 + n_z - 1)
    for k in range(3):
        square_copy(0, k).start()

    route_t[...] = routes_ref[...].T
    weight_t[...] = weights_ref[...].T
    lane = iota((tok, 128), 1)
    group = route_t[pl.ds(me * tok, tok), :][:, 0:1] // GROUP
    in_group = (lane == group).astype(F32)
    before = (iota((tok, tok), 1) < iota((tok, tok), 0)).astype(BF16)
    ranks = jnp.dot(before, in_group.astype(BF16), preferred_element_type=F32)
    rank = jnp.sum(ranks * in_group, axis=1, keepdims=True).astype(jnp.int32)
    place = jnp.where(group == chips[0], 0, -1)
    for d in range(1, n_z):
        place = jnp.where(group == chips[d], d, place)
    own_lane = iota((tok, n_z * rows_z), 1)
    own_pick[...] = (own_lane == place * rows_z + rank).astype(BF16)

    def prepare(d):
        routes = route_t[pl.ds(chips[d] * pair, pair), :]
        weights = weight_t[pl.ds(chips[d] * pair, pair), :]
        lane = iota((pair, 128), 1)
        row = iota((pair, 128), 0)
        first = me * n_exp
        hits = jnp.where((lane == n_exp) & (routes[:, 0:1] // GROUP == z), 1.0, 0.0)
        wt = jnp.zeros((pair, 128), F32)
        for k in range(top):
            match = (routes[:, k : k + 1] == first + lane) & (lane < n_exp)
            hits = hits + jnp.where(match, 1.0, 0.0)
            wt = wt + jnp.where(match, weights[:, k : k + 1], 0.0)
        t_row, t_col = iota((pair, pair), 0), iota((pair, pair), 1)
        before = ((t_col < t_row) & (t_col // tok == t_row // tok)).astype(BF16)
        ranks = jnp.dot(before, hits.astype(BF16), preferred_element_type=F32)
        rank = jnp.where(hits > 0.0, ranks, -1.0).astype(jnp.int32)
        wide = iota((pair, 2 * rows_z), 1)
        wide_core = iota((pair, 2 * rows_z), 0) // tok
        group_rows = (
            (rank[:, n_exp : n_exp + 1] == wide % rows_z) & (wide // rows_z == wide_core)
        ).astype(BF16)
        slots = n_exp * 2 * cap
        lane = iota((pair, slots), 1)
        row = iota((pair, slots), 0)
        expert_rank = jnp.broadcast_to(rank[:, 0:1], (pair, slots))
        for j in range(1, n_exp):
            expert_rank = jnp.where(lane // (2 * cap) == j, rank[:, j : j + 1], expert_rank)
        slot = (
            (expert_rank == lane % cap) & ((lane // cap) % 2 == row // tok)
        ).astype(BF16)
        pick[d] = tdot(slot, group_rows).astype(BF16)
        w_hi = wt.astype(BF16)
        w_mid = (wt - w_hi.astype(F32)).astype(BF16)
        w_lo = (wt - w_hi.astype(F32) - w_mid.astype(F32)).astype(BF16)
        weight = tdot(slot, w_hi) + tdot(slot, w_mid) + tdot(slot, w_lo)
        weight = jnp.where(
            iota((slots, 128), 1) == iota((slots, 128), 0) // (2 * cap), weight, 0.0
        )
        weight = jnp.broadcast_to(jnp.sum(weight, axis=1, keepdims=True), (slots, 128))
        weight = weight.reshape(n_exp, 2 * cap, 128)
        for i, chunk in enumerate(chunks):
            if d in chunk:
                at = chunk.index(d) * 2 * cap
                slot_w[i, :, at : at + 2 * cap, :] = weight

    prepare(0)

    for k in range(3):
        square_copy(0, k).wait_recv()
    square = ss_out[0] + ss_in[0, 0] + ss_in[0, 1] + ss_in[0, 2]
    scale = lax.rsqrt(square[:, 0:1] / D + EPS)
    normed = (values * scale * in_gain_ref[...]).astype(BF16)
    send_rows[...] = tdot(own_pick[...], normed).astype(BF16).reshape(n_z, rows_z, width)

    def dispatch(d):
        return remote(
            send_rows.at[d], compact.at[d, core], d_send.at[d], d_recv.at[d], "ep", far_ep(d)
        )

    def forward(d):
        src = compact.at[d, core] if d else send_rows.at[0]
        return remote(src, compact.at[d, core], f_send.at[d], f_recv.at[d], "ep", partner)

    forward(0).start()
    for d in far_order:
        dispatch(d).start()
    compact[0, core] = send_rows[0]

    def side(h):
        return (x_tp, y_tp, x, y) if h == 0 else (y_tp, x_tp, y, x)

    def hop(i, stage, j, h):
        near, next_near, a, b = side(h)
        _, part, s1_in, _, s2_out, s2_in, act, _, _ = bufs[i]
        send, recv = sems[i][2 * stage].at[j, h], sems[i][2 * stage + 1].at[j, h]
        if stage == 0:
            src, dst, to = part.at[j, pl.ds(h * 4 + 2 * (1 - a), 2)], s1_in.at[j, h], near
        elif stage == 1:
            src, dst, to = s2_out.at[j, h], s2_in.at[j, h], next_near
        elif stage == 2:
            src, to = act.at[j, h * 4 + 2 * a + b], next_near
            dst = src
        else:
            src, to = act.at[j, pl.ds(h * 4 + 2 * a, 2)], near
            dst = src
        return remote(src, dst, send, recv, "tp", to)

    def w_wait(k, j, hbm, vmem):
        pltpu.make_async_copy(hbm.at[j], vmem.at[j], w_sem.at[k, j]).wait()

    def project(i, send):
        chunk = chunks[i]
        xs, part = bufs[i][0], bufs[i][1]
        for at, d in enumerate(chunk):
            rows = compact[d].reshape(2 * rows_z, width)
            picked = jnp.dot(pick[d], rows, preferred_element_type=F32).astype(BF16)
            xs[:, at * 2 * cap : (at + 1) * 2 * cap, :] = picked.reshape(n_exp, 2 * cap, width)

        @pl.loop(0, n_exp)
        def _(j):
            for k, (hbm, vmem) in enumerate(((wg_hbm, wg), (wu_hbm, wu))):
                if i == 0:
                    w_wait(k, j, hbm, vmem)
                result = jnp.dot(xs[j], vmem[j], preferred_element_type=F32).astype(BF16)
                for p in range(8):
                    part[j, p, k] = result[:, p * piece_cols : (p + 1) * piece_cols]
            if send:
                for h in range(2):
                    hop(i, 0, j, h).start()

    def send_parts(i):
        @pl.loop(0, n_exp)
        def _(j):
            for h in range(2):
                hop(i, 0, j, h).start()

    def add_first(i):
        _, part, s1_in, keep, s2_out = bufs[i][:5]

        @pl.loop(0, n_exp)
        def _(j):
            for h in range(2):
                _, _, a, b = side(h)
                hop(i, 0, j, h).wait_recv()
                mine = h * 4 + 2 * a
                s2_out[j, h] = (
                    part[j, mine + 1 - b].astype(F32) + s1_in[j, h, 1 - b].astype(F32)
                ).astype(BF16)
                hop(i, 1, j, h).start()
                keep[j, h] = part[j, mine + b].astype(F32) + s1_in[j, h, b].astype(F32)

    def activate(i):
        _, _, _, keep, _, s2_in, act = bufs[i][:7]
        rows = act.shape[2]

        @pl.loop(0, n_exp)
        def _(j):
            for h in range(2):
                _, _, a, b = side(h)
                hop(i, 1, j, h).wait_recv()
                total = keep[j, h] + s2_in[j, h].astype(F32)
                gate, up = total[0], total[1]
                act[j, h * 4 + 2 * a + b] = (
                    gate / (1.0 + jnp.exp(-gate)) * up * slot_w[i, j, 0:rows, 0:1]
                ).astype(BF16)
                hop(i, 2, j, h).start()

    def pass_on(i):
        @pl.loop(0, n_exp)
        def _(j):
            for h in range(2):
                hop(i, 2, j, h).wait_recv()
                hop(i, 3, j, h).start()

    def swap(d):
        return remote(x_out.at[d], x_in.at[d], x_send.at[d], x_recv.at[d], "ep", partner)

    def home(d):
        return remote(r_out.at[d], r_in.at[d], r_send.at[d], r_recv.at[d], "ep", far_ep(d))

    def down(i):
        act, res, comb = bufs[i][6:]

        @pl.loop(0, n_exp)
        def _(j):
            if i == 0:
                w_wait(2, j, wd_hbm, wd)
            for h in range(2):
                hop(i, 3, j, h).wait_recv()
            rows = jnp.concatenate([act[j, p] for p in range(8)], axis=1)
            res[j] = jnp.dot(rows, wd[j], preferred_element_type=F32).astype(BF16)

        for at, d in enumerate(chunks[i]):
            result = res[:, at * 2 * cap : (at + 1) * 2 * cap, :]
            result = result.reshape(n_exp * 2 * cap, width)
            comb[at] = tdot(pick[d], result).reshape(2, rows_z, width)
            x_out[d] = comb[at, other].astype(BF16)
            swap(d).start()

    def send_home(i):
        comb = bufs[i][8]
        for at, d in enumerate(chunks[i]):
            swap(d).wait_recv()
            total = (comb[at, core] + x_in[d].astype(F32)).astype(BF16)
            if d:
                r_out[d] = total
                home(d).start()
            else:
                r_in[0] = total

    def received(d):
        return remote(
            compact.at[d, core], compact.at[d, other], f_send.at[d], f_recv.at[d], "ep", partner
        )

    received(0).wait_recv()
    project(0, True)
    for d in far_order:
        prepare(d)
    add_first(0)
    activate(0)
    for d in far_order:
        dispatch(d).wait_recv()
        forward(d).start()
    pass_on(0)
    for d in chunks[1]:
        received(d).wait_recv()
    project(1, True)
    for d in chunks[2]:
        received(d).wait_recv()
    project(2, False)
    down(0)
    add_first(1)
    send_home(0)
    activate(1)
    send_parts(2)
    pass_on(1)
    add_first(2)
    activate(2)
    down(1)
    pass_on(2)
    send_home(1)
    down(2)
    send_home(2)
    for d in far_order:
        home(d).wait_recv()

    combined = jnp.dot(
        own_pick[...], r_in[...].reshape(n_z * rows_z, width), preferred_element_type=F32
    )
    square = jnp.sum(combined * combined, axis=1, keepdims=True)
    ss_out[1] = jnp.broadcast_to(square, (tok, 128))
    for k in range(3):
        square_copy(1, k).start()
    for k in range(3):
        square_copy(1, k).wait_recv()
    square = ss_out[1] + ss_in[1, 0] + ss_in[1, 1] + ss_in[1, 2]
    scale = lax.rsqrt(square[:, 0:1] / D + EPS)
    out_ref[...] = (combined * scale * out_gain_ref[...]).astype(BF16)

    for k in range(3):
        square_copy(0, k).wait_send()
        square_copy(1, k).wait_send()
    for d in range(n_z):
        forward(d).wait_send()
        swap(d).wait_send()
        if d:
            dispatch(d).wait_send()
            home(d).wait_send()

    @pl.loop(0, n_exp)
    def _(j):
        for i in range(len(chunks)):
            for h in range(2):
                for stage in range(4):
                    hop(i, stage, j, h).wait_send()


CHUNKS = ((0,), (2, 3), (1,))


def fused(mesh, tokens, in_gain, out_gain, routes, route_weights, w_gate, w_up, w_down):
    tok, width = tokens.shape
    tok_all, top = routes.shape
    n_exp, _, ff = w_gate.shape
    n_ep = mesh.shape["ep"]
    n_z = n_ep // 2
    cap = max(2, 2 * tok * top // (n_exp * n_ep))
    rows_z = cap * GROUP // top
    cfg = (n_z, tok, n_exp, cap, width, ff, top, CHUNKS)
    vmem = pl.BlockSpec(memory_space=pltpu.VMEM)
    hbm = pl.BlockSpec(memory_space=pl.ANY)
    dma = pltpu.SemaphoreType.DMA
    longest = max(len(chunk) for chunk in CHUNKS)
    scratch = [
        pltpu.VMEM(w_gate.shape, BF16),
        pltpu.VMEM(w_up.shape, BF16),
        pltpu.VMEM(w_down.shape, BF16),
        pltpu.VMEM((tok_all, top), jnp.int32),
        pltpu.VMEM((tok_all, top), F32),
        pltpu.VMEM((n_z, n_exp * 2 * cap, 2 * rows_z), BF16),
        pltpu.VMEM((len(CHUNKS), n_exp, longest * 2 * cap, 128), F32),
        pltpu.VMEM((tok, n_z * rows_z), BF16),
        pltpu.VMEM((2, tok, 128), F32),
        pltpu.VMEM((2, 3, tok, 128), F32),
        pltpu.VMEM((n_z, rows_z, width), BF16),
        pltpu.VMEM((n_z, 2, rows_z, width), BF16),
    ] + [pltpu.VMEM((n_z, rows_z, width), BF16)] * 4
    for chunk in CHUNKS:
        rows = len(chunk) * 2 * cap
        cols = ff // 8
        scratch += [
            pltpu.VMEM((n_exp, rows, width), BF16),
            pltpu.VMEM((n_exp, 8, 2, rows, cols), BF16),
            pltpu.VMEM((n_exp, 2, 2, 2, rows, cols), BF16),
            pltpu.VMEM((n_exp, 2, 2, rows, cols), F32),
            pltpu.VMEM((n_exp, 2, 2, rows, cols), BF16),
            pltpu.VMEM((n_exp, 2, 2, rows, cols), BF16),
            pltpu.VMEM((n_exp, 8, rows, cols), BF16),
            pltpu.VMEM((n_exp, rows, width), BF16),
            pltpu.VMEM((len(chunk), 2, rows_z, width), F32),
        ]
    scratch += [dma((3, n_exp)), dma((2, 3)), dma((2, 3))]
    scratch += [dma((n_z,))] * 8
    scratch += [dma((n_exp, 2))] * (8 * len(CHUNKS))
    return pl.pallas_call(
        functools.partial(kernel, cfg),
        out_shape=jax.ShapeDtypeStruct((tok, width), BF16),
        in_specs=[vmem] * 5 + [hbm] * 3,
        out_specs=vmem,
        scratch_shapes=scratch,
        compiler_params=pltpu.CompilerParams(
            collective_id=0, has_side_effects=True, vmem_limit_bytes=60 * 2**20
        ),
    )(
        tokens,
        in_gain.reshape(1, width),
        out_gain.reshape(1, width),
        routes.T,
        route_weights.T,
        w_gate,
        w_up,
        w_down,
    )


def run_experts(slot_rows, w_gate, w_up, w_down):
    gate_part = jnp.einsum(
        "secd,edf->secf", slot_rows, w_gate, preferred_element_type=jnp.float32
    ).astype(jnp.bfloat16)
    up_part = jnp.einsum(
        "secd,edf->secf", slot_rows, w_up, preferred_element_type=jnp.float32
    ).astype(jnp.bfloat16)
    gate_sum, up_sum = (
        lax.psum(gate_part, "tp").astype(jnp.float32),
        lax.psum(up_part, "tp").astype(jnp.float32),
    )
    active = (jax.nn.silu(gate_sum) * up_sum).astype(jnp.bfloat16)
    return jnp.einsum("secf,efd->secd", active, w_down, preferred_element_type=jnp.float32).astype(
        jnp.bfloat16
    )


def on_device(tokens, in_gain, out_gain, routes, route_weights, w_gate, w_up, w_down):
    tok_rows, local_width = tokens.shape
    top_count = routes.shape[1]
    local_experts = w_gate.shape[0]
    groups_ep = lax.axis_size("ep")
    experts = local_experts * groups_ep
    capacity = max(2, 2 * tok_rows * top_count // experts)
    values = tokens.astype(jnp.float32)
    sum_squares = lax.psum(jnp.sum(values * values, axis=1), "tp")
    normed = (values * lax.rsqrt(sum_squares / D + EPS)[:, None] * in_gain).astype(jnp.bfloat16)
    row_start = lax.axis_index("ep") * tok_rows
    my_routes = lax.dynamic_slice_in_dim(routes, row_start, tok_rows, 0)
    my_weights = lax.dynamic_slice_in_dim(route_weights, row_start, tok_rows, 0)
    flat_ids = my_routes.reshape(-1)
    matches = (flat_ids[:, None] == jnp.arange(experts, dtype=jnp.int32)[None, :]).astype(jnp.int32)
    slot_rank = jnp.sum((jnp.cumsum(matches, axis=0) - matches) * matches, axis=1)
    position = flat_ids * capacity + slot_rank
    dispatch_table = jnp.any(
        position.reshape(tok_rows, top_count, 1)
        == jnp.arange(experts * capacity, dtype=jnp.int32)[None, None, :],
        axis=1,
    )
    outgoing = jnp.einsum(
        "ts,td->sd", dispatch_table.astype(jnp.bfloat16), normed, preferred_element_type=jnp.float32
    ).astype(jnp.bfloat16)
    outgoing = outgoing.reshape(groups_ep, local_experts, capacity, local_width)
    answers = run_experts(
        lax.all_to_all(outgoing, "ep", split_axis=0, concat_axis=0, tiled=True),
        w_gate,
        w_up,
        w_down,
    )
    returned = lax.all_to_all(answers, "ep", split_axis=0, concat_axis=0, tiled=True)
    flat_out = returned.reshape(experts * capacity, local_width)
    picked = flat_out[position].reshape(tok_rows, top_count, local_width)
    combined = jnp.sum(my_weights[:, :, None] * picked.astype(jnp.float32), axis=1)
    out_squares = lax.psum(jnp.sum(combined * combined, axis=1), "tp")
    return (combined * lax.rsqrt(out_squares / D + EPS)[:, None] * out_gain).astype(jnp.bfloat16)


def solution(mesh):
    placed = (
        P("ep", "tp"),
        P("tp"),
        P("tp"),
        P(),
        P(),
        P("ep", "tp", None),
        P("ep", "tp", None),
        P("ep", None, "tp"),
    )
    body = on_device
    if mesh.shape["tp"] == 4 and mesh.shape["ep"] == 8:
        body = functools.partial(fused, mesh)
    return jax.shard_map(
        body, mesh=mesh, in_specs=placed, out_specs=P("ep", "tp"), check_vma=False
    )
```

```python
import functools

import jax
import jax.numpy as jnp
from jax import lax
from jax.experimental import pallas as pl
from jax.experimental.pallas import tpu as pltpu
from jax.sharding import PartitionSpec as P

D = 4096
GROUP = 8

EPS = 1e-06
MESH = pl.DeviceIdType.MESH
F32, BF16 = jnp.float32, jnp.bfloat16


def iota(shape, dim):
    return lax.broadcasted_iota(jnp.int32, shape, dim)


def tdot(a, b):
    return lax.dot_general(a, b, (((0,), (0,)), ((), ())), preferred_element_type=F32)


def kernel(cfg, *refs):
    n_z, tok, n_exp, cap, width, ff, top, chunks = cfg
    it = iter(refs)
    tokens_ref, in_gain_ref, out_gain_ref, routes_ref, weights_ref = [next(it) for _ in range(5)]
    wg_hbm, wu_hbm, wd_hbm, out_ref, wg, wu, wd = [next(it) for _ in range(7)]
    route_t, weight_t, pick, slot_w, own_pick = [next(it) for _ in range(5)]
    ss_out, ss_in, send_rows, compact, x_out, x_in, r_out, r_in = [next(it) for _ in range(8)]
    bufs = [[next(it) for _ in range(9)] for _ in chunks]
    w_sem, ss_send, ss_recv, d_send, f_send, d_recv, f_recv = [next(it) for _ in range(7)]
    x_send, x_recv, r_send, r_recv = [next(it) for _ in range(4)]
    sems = [[next(it) for _ in range(8)] for _ in chunks]

    rows_z = cap * GROUP // top
    pair = 2 * tok
    piece_cols = ff // 8
    me = lax.axis_index("ep")
    tp = lax.axis_index("tp")
    z, core = me // 2, lax.rem(me, 2)
    other = 1 - core
    y, x = tp // 2, lax.rem(tp, 2)
    x_tp = 2 * y + (1 - x)
    y_tp = 2 * (1 - y) + x
    xy_tp = 2 * (1 - y) + (1 - x)
    partner = 2 * z + other
    peers = (x_tp, y_tp, xy_tp)
    chips = (z, z + 1 - 2 * lax.rem(z, 2), lax.rem(z + 2, n_z), n_z - 1 - z)
    far_order = range(1, n_z)

    for j in range(n_exp):
        pltpu.make_async_copy(wg_hbm.at[j], wg.at[j], w_sem.at[0, j]).start()
        pltpu.make_async_copy(wu_hbm.at[j], wu.at[j], w_sem.at[1, j]).start()
    for j in range(n_exp):
        pltpu.make_async_copy(wd_hbm.at[j], wd.at[j], w_sem.at[2, j]).start()

    def far_ep(d):
        return 2 * chips[d] + core

    barrier = pltpu.get_barrier_semaphore()
    for peer in peers:
        pl.semaphore_signal(barrier, inc=1, device_id={"tp": peer}, device_id_type=MESH)
    pl.semaphore_signal(barrier, inc=1, device_id={"ep": partner}, device_id_type=MESH)
    for d in far_order:
        pl.semaphore_signal(barrier, inc=1, device_id={"ep": far_ep(d)}, device_id_type=MESH)

    def remote(src, dst, send, recv, axis, dev):
        return pltpu.make_async_remote_copy(
            src_ref=src,
            dst_ref=dst,
            send_sem=send,
            recv_sem=recv,
            device_id={axis: dev},
            device_id_type=MESH,
        )

    def square_copy(which, k):
        return remote(
            ss_out.at[which],
            ss_in.at[which, k],
            ss_send.at[which, k],
            ss_recv.at[which, k],
            "tp",
            peers[k],
        )

    values = tokens_ref[...].astype(F32)
    square = jnp.sum(values * values, axis=1, keepdims=True)
    ss_out[0] = jnp.broadcast_to(square, (tok, 128))
    pl.semaphore_wait(barrier, 4 + n_z - 1)
    for k in range(3):
        square_copy(0, k).start()

    route_t[...] = routes_ref[...].T
    weight_t[...] = weights_ref[...].T
    lane = iota((tok, 128), 1)
    group = route_t[pl.ds(me * tok, tok), :][:, 0:1] // GROUP
    in_group = (lane == group).astype(F32)
    before = (iota((tok, tok), 1) < iota((tok, tok), 0)).astype(BF16)
    ranks = jnp.dot(before, in_group.astype(BF16), preferred_element_type=F32)
    rank = jnp.sum(ranks * in_group, axis=1, keepdims=True).astype(jnp.int32)
    place = jnp.where(group == chips[0], 0, -1)
    for d in range(1, n_z):
        place = jnp.where(group == chips[d], d, place)
    own_lane = iota((tok, n_z * rows_z), 1)
    own_pick[...] = (own_lane == place * rows_z + rank).astype(BF16)

    def prepare(d):
        routes = route_t[pl.ds(chips[d] * pair, pair), :]
        weights = weight_t[pl.ds(chips[d] * pair, pair), :]
        lane = iota((pair, 128), 1)
        row = iota((pair, 128), 0)
        first = me * n_exp
        hits = jnp.where((lane == n_exp) & (routes[:, 0:1] // GROUP == z), 1.0, 0.0)
        wt = jnp.zeros((pair, 128), F32)
        for k in range(top):
            match = (routes[:, k : k + 1] == first + lane) & (lane < n_exp)
            hits = hits + jnp.where(match, 1.0, 0.0)
            wt = wt + jnp.where(match, weights[:, k : k + 1], 0.0)
        t_row, t_col = iota((pair, pair), 0), iota((pair, pair), 1)
        before = ((t_col < t_row) & (t_col // tok == t_row // tok)).astype(BF16)
        ranks = jnp.dot(before, hits.astype(BF16), preferred_element_type=F32)
        rank = jnp.where(hits > 0.0, ranks, -1.0).astype(jnp.int32)
        wide = iota((pair, 2 * rows_z), 1)
        wide_core = iota((pair, 2 * rows_z), 0) // tok
        group_rows = (
            (rank[:, n_exp : n_exp + 1] == wide % rows_z) & (wide // rows_z == wide_core)
        ).astype(BF16)
        slots = n_exp * 2 * cap
        lane = iota((pair, slots), 1)
        row = iota((pair, slots), 0)
        expert_rank = jnp.broadcast_to(rank[:, 0:1], (pair, slots))
        for j in range(1, n_exp):
            expert_rank = jnp.where(lane // (2 * cap) == j, rank[:, j : j + 1], expert_rank)
        slot = (
            (expert_rank == lane % cap) & ((lane // cap) % 2 == row // tok)
        ).astype(BF16)
        pick[d] = tdot(slot, group_rows).astype(BF16)
        w_hi = wt.astype(BF16)
        w_mid = (wt - w_hi.astype(F32)).astype(BF16)
        w_lo = (wt - w_hi.astype(F32) - w_mid.astype(F32)).astype(BF16)
        weight = tdot(slot, w_hi) + tdot(slot, w_mid) + tdot(slot, w_lo)
        weight = jnp.where(
            iota((slots, 128), 1) == iota((slots, 128), 0) // (2 * cap), weight, 0.0
        )
        weight = jnp.broadcast_to(jnp.sum(weight, axis=1, keepdims=True), (slots, 128))
        weight = weight.reshape(n_exp, 2 * cap, 128)
        for i, chunk in enumerate(chunks):
            if d in chunk:
                at = chunk.index(d) * 2 * cap
                slot_w[i, :, at : at + 2 * cap, :] = weight

    prepare(0)

    for k in range(3):
        square_copy(0, k).wait_recv()
    square = ss_out[0] + ss_in[0, 0] + ss_in[0, 1] + ss_in[0, 2]
    scale = lax.rsqrt(square[:, 0:1] / D + EPS)
    normed = (values * scale * in_gain_ref[...]).astype(BF16)
    send_rows[...] = tdot(own_pick[...], normed).astype(BF16).reshape(n_z, rows_z, width)

    def dispatch(d):
        return remote(
            send_rows.at[d], compact.at[d, core], d_send.at[d], d_recv.at[d], "ep", far_ep(d)
        )

    def forward(d):
        src = compact.at[d, core] if d else send_rows.at[0]
        return remote(src, compact.at[d, core], f_send.at[d], f_recv.at[d], "ep", partner)

    forward(0).start()
    for d in far_order:
        dispatch(d).start()
    compact[0, core] = send_rows[0]

    def side(h):
        return (x_tp, y_tp, x, y) if h == 0 else (y_tp, x_tp, y, x)

    def hop(i, stage, j, h):
        near, next_near, a, b = side(h)
        _, part, s1_in, _, s2_out, s2_in, act, _, _ = bufs[i]
        send, recv = sems[i][2 * stage].at[j, h], sems[i][2 * stage + 1].at[j, h]
        if stage == 0:
            src, dst, to = part.at[j, pl.ds(h * 4 + 2 * (1 - a), 2)], s1_in.at[j, h], near
        elif stage == 1:
            src, dst, to = s2_out.at[j, h], s2_in.at[j, h], next_near
        elif stage == 2:
            src, to = act.at[j, h * 4 + 2 * a + b], next_near
            dst = src
        else:
            src, to = act.at[j, pl.ds(h * 4 + 2 * a, 2)], near
            dst = src
        return remote(src, dst, send, recv, "tp", to)

    def w_wait(k, j, hbm, vmem):
        pltpu.make_async_copy(hbm.at[j], vmem.at[j], w_sem.at[k, j]).wait()

    def project(i):
        chunk = chunks[i]
        xs, part = bufs[i][0], bufs[i][1]
        for at, d in enumerate(chunk):
            rows = compact[d].reshape(2 * rows_z, width)
            picked = jnp.dot(pick[d], rows, preferred_element_type=F32).astype(BF16)
            xs[:, at * 2 * cap : (at + 1) * 2 * cap, :] = picked.reshape(n_exp, 2 * cap, width)

        @pl.loop(0, n_exp)
        def _(j):
            for k, (hbm, vmem) in enumerate(((wg_hbm, wg), (wu_hbm, wu))):
                if i == 0:
                    w_wait(k, j, hbm, vmem)
                result = jnp.dot(xs[j], vmem[j], preferred_element_type=F32).astype(BF16)
                for p in range(8):
                    part[j, p, k] = result[:, p * piece_cols : (p + 1) * piece_cols]
            for h in range(2):
                hop(i, 0, j, h).start()

    def add_first(i):
        _, part, s1_in, keep, s2_out = bufs[i][:5]

        @pl.loop(0, n_exp)
        def _(j):
            for h in range(2):
                _, _, a, b = side(h)
                hop(i, 0, j, h).wait_recv()
                mine = h * 4 + 2 * a
                s2_out[j, h] = (
                    part[j, mine + 1 - b].astype(F32) + s1_in[j, h, 1 - b].astype(F32)
                ).astype(BF16)
                hop(i, 1, j, h).start()
                keep[j, h] = part[j, mine + b].astype(F32) + s1_in[j, h, b].astype(F32)

    def activate(i):
        _, _, _, keep, _, s2_in, act = bufs[i][:7]
        rows = act.shape[2]

        @pl.loop(0, n_exp)
        def _(j):
            for h in range(2):
                _, _, a, b = side(h)
                hop(i, 1, j, h).wait_recv()
                total = keep[j, h] + s2_in[j, h].astype(F32)
                gate, up = total[0], total[1]
                act[j, h * 4 + 2 * a + b] = (
                    gate / (1.0 + jnp.exp(-gate)) * up * slot_w[i, j, 0:rows, 0:1]
                ).astype(BF16)
                hop(i, 2, j, h).start()

    def pass_on(i):
        @pl.loop(0, n_exp)
        def _(j):
            for h in range(2):
                hop(i, 2, j, h).wait_recv()
                hop(i, 3, j, h).start()

    def swap(d):
        return remote(x_out.at[d], x_in.at[d], x_send.at[d], x_recv.at[d], "ep", partner)

    def home(d):
        return remote(r_out.at[d], r_in.at[d], r_send.at[d], r_recv.at[d], "ep", far_ep(d))

    def down(i):
        act, res, comb = bufs[i][6:]

        @pl.loop(0, n_exp)
        def _(j):
            if i == 0:
                w_wait(2, j, wd_hbm, wd)
            for h in range(2):
                hop(i, 3, j, h).wait_recv()
            rows = jnp.concatenate([act[j, p] for p in range(8)], axis=1)
            res[j] = jnp.dot(rows, wd[j], preferred_element_type=F32).astype(BF16)

        for at, d in enumerate(chunks[i]):
            result = res[:, at * 2 * cap : (at + 1) * 2 * cap, :]
            result = result.reshape(n_exp * 2 * cap, width)
            comb[at] = tdot(pick[d], result).reshape(2, rows_z, width)
            x_out[d] = comb[at, other].astype(BF16)
            swap(d).start()

    def send_home(i):
        comb = bufs[i][8]
        for at, d in enumerate(chunks[i]):
            swap(d).wait_recv()
            total = (comb[at, core] + x_in[d].astype(F32)).astype(BF16)
            if d:
                r_out[d] = total
                home(d).start()
            else:
                r_in[0] = total

    def received(d):
        return remote(
            compact.at[d, core], compact.at[d, other], f_send.at[d], f_recv.at[d], "ep", partner
        )

    def relay(d):
        dispatch(d).wait_recv()
        forward(d).start()

    own, far, near = range(3)
    received(0).wait_recv()
    project(own)
    for d in chunks[near]:
        prepare(d)
        relay(d)
    add_first(own)
    for d in chunks[near]:
        received(d).wait_recv()
    project(near)
    for d in chunks[far]:
        prepare(d)
    activate(own)
    for d in chunks[far]:
        relay(d)
    for d in chunks[far]:
        received(d).wait_recv()
    project(far)
    pass_on(own)
    add_first(near)
    add_first(far)
    activate(near)
    down(own)
    activate(far)
    pass_on(far)
    send_home(own)
    pass_on(near)
    down(far)
    send_home(far)
    down(near)
    send_home(near)
    for d in far_order:
        home(d).wait_recv()

    combined = jnp.dot(
        own_pick[...], r_in[...].reshape(n_z * rows_z, width), preferred_element_type=F32
    )
    square = jnp.sum(combined * combined, axis=1, keepdims=True)
    ss_out[1] = jnp.broadcast_to(square, (tok, 128))
    for k in range(3):
        square_copy(1, k).start()
    for k in range(3):
        square_copy(1, k).wait_recv()
    square = ss_out[1] + ss_in[1, 0] + ss_in[1, 1] + ss_in[1, 2]
    scale = lax.rsqrt(square[:, 0:1] / D + EPS)
    out_ref[...] = (combined * scale * out_gain_ref[...]).astype(BF16)

    for k in range(3):
        square_copy(0, k).wait_send()
        square_copy(1, k).wait_send()
    for d in range(n_z):
        forward(d).wait_send()
        swap(d).wait_send()
        if d:
            dispatch(d).wait_send()
            home(d).wait_send()

    @pl.loop(0, n_exp)
    def _(j):
        for i in range(len(chunks)):
            for h in range(2):
                for stage in range(4):
                    hop(i, stage, j, h).wait_send()


CHUNKS = ((0,), (2, 3), (1,))


def fused(mesh, tokens, in_gain, out_gain, routes, route_weights, w_gate, w_up, w_down):
    tok, width = tokens.shape
    tok_all, top = routes.shape
    n_exp, _, ff = w_gate.shape
    n_ep = mesh.shape["ep"]
    n_z = n_ep // 2
    cap = max(2, 2 * tok * top // (n_exp * n_ep))
    rows_z = cap * GROUP // top
    cfg = (n_z, tok, n_exp, cap, width, ff, top, CHUNKS)
    vmem = pl.BlockSpec(memory_space=pltpu.VMEM)
    hbm = pl.BlockSpec(memory_space=pl.ANY)
    dma = pltpu.SemaphoreType.DMA
    longest = max(len(chunk) for chunk in CHUNKS)
    scratch = [
        pltpu.VMEM(w_gate.shape, BF16),
        pltpu.VMEM(w_up.shape, BF16),
        pltpu.VMEM(w_down.shape, BF16),
        pltpu.VMEM((tok_all, top), jnp.int32),
        pltpu.VMEM((tok_all, top), F32),
        pltpu.VMEM((n_z, n_exp * 2 * cap, 2 * rows_z), BF16),
        pltpu.VMEM((len(CHUNKS), n_exp, longest * 2 * cap, 128), F32),
        pltpu.VMEM((tok, n_z * rows_z), BF16),
        pltpu.VMEM((2, tok, 128), F32),
        pltpu.VMEM((2, 3, tok, 128), F32),
        pltpu.VMEM((n_z, rows_z, width), BF16),
        pltpu.VMEM((n_z, 2, rows_z, width), BF16),
    ] + [pltpu.VMEM((n_z, rows_z, width), BF16)] * 4
    for chunk in CHUNKS:
        rows = len(chunk) * 2 * cap
        cols = ff // 8
        scratch += [
            pltpu.VMEM((n_exp, rows, width), BF16),
            pltpu.VMEM((n_exp, 8, 2, rows, cols), BF16),
            pltpu.VMEM((n_exp, 2, 2, 2, rows, cols), BF16),
            pltpu.VMEM((n_exp, 2, 2, rows, cols), F32),
            pltpu.VMEM((n_exp, 2, 2, rows, cols), BF16),
            pltpu.VMEM((n_exp, 2, 2, rows, cols), BF16),
            pltpu.VMEM((n_exp, 8, rows, cols), BF16),
            pltpu.VMEM((n_exp, rows, width), BF16),
            pltpu.VMEM((len(chunk), 2, rows_z, width), F32),
        ]
    scratch += [dma((3, n_exp)), dma((2, 3)), dma((2, 3))]
    scratch += [dma((n_z,))] * 8
    scratch += [dma((n_exp, 2))] * (8 * len(CHUNKS))
    return pl.pallas_call(
        functools.partial(kernel, cfg),
        out_shape=jax.ShapeDtypeStruct((tok, width), BF16),
        in_specs=[vmem] * 5 + [hbm] * 3,
        out_specs=vmem,
        scratch_shapes=scratch,
        compiler_params=pltpu.CompilerParams(
            collective_id=0, has_side_effects=True, vmem_limit_bytes=60 * 2**20
        ),
    )(
        tokens,
        in_gain.reshape(1, width),
        out_gain.reshape(1, width),
        routes.T,
        route_weights.T,
        w_gate,
        w_up,
        w_down,
    )


def run_experts(slot_rows, w_gate, w_up, w_down):
    gate_part = jnp.einsum(
        "secd,edf->secf", slot_rows, w_gate, preferred_element_type=jnp.float32
    ).astype(jnp.bfloat16)
    up_part = jnp.einsum(
        "secd,edf->secf", slot_rows, w_up, preferred_element_type=jnp.float32
    ).astype(jnp.bfloat16)
    gate_sum, up_sum = (
        lax.psum(gate_part, "tp").astype(jnp.float32),
        lax.psum(up_part, "tp").astype(jnp.float32),
    )
    active = (jax.nn.silu(gate_sum) * up_sum).astype(jnp.bfloat16)
    return jnp.einsum("secf,efd->secd", active, w_down, preferred_element_type=jnp.float32).astype(
        jnp.bfloat16
    )


def on_device(tokens, in_gain, out_gain, routes, route_weights, w_gate, w_up, w_down):
    tok_rows, local_width = tokens.shape
    top_count = routes.shape[1]
    local_experts = w_gate.shape[0]
    groups_ep = lax.axis_size("ep")
    experts = local_experts * groups_ep
    capacity = max(2, 2 * tok_rows * top_count // experts)
    values = tokens.astype(jnp.float32)
    sum_squares = lax.psum(jnp.sum(values * values, axis=1), "tp")
    normed = (values * lax.rsqrt(sum_squares / D + EPS)[:, None] * in_gain).astype(jnp.bfloat16)
    row_start = lax.axis_index("ep") * tok_rows
    my_routes = lax.dynamic_slice_in_dim(routes, row_start, tok_rows, 0)
    my_weights = lax.dynamic_slice_in_dim(route_weights, row_start, tok_rows, 0)
    flat_ids = my_routes.reshape(-1)
    matches = (flat_ids[:, None] == jnp.arange(experts, dtype=jnp.int32)[None, :]).astype(jnp.int32)
    slot_rank = jnp.sum((jnp.cumsum(matches, axis=0) - matches) * matches, axis=1)
    position = flat_ids * capacity + slot_rank
    dispatch_table = jnp.any(
        position.reshape(tok_rows, top_count, 1)
        == jnp.arange(experts * capacity, dtype=jnp.int32)[None, None, :],
        axis=1,
    )
    outgoing = jnp.einsum(
        "ts,td->sd", dispatch_table.astype(jnp.bfloat16), normed, preferred_element_type=jnp.float32
    ).astype(jnp.bfloat16)
    outgoing = outgoing.reshape(groups_ep, local_experts, capacity, local_width)
    answers = run_experts(
        lax.all_to_all(outgoing, "ep", split_axis=0, concat_axis=0, tiled=True),
        w_gate,
        w_up,
        w_down,
    )
    returned = lax.all_to_all(answers, "ep", split_axis=0, concat_axis=0, tiled=True)
    flat_out = returned.reshape(experts * capacity, local_width)
    picked = flat_out[position].reshape(tok_rows, top_count, local_width)
    combined = jnp.sum(my_weights[:, :, None] * picked.astype(jnp.float32), axis=1)
    out_squares = lax.psum(jnp.sum(combined * combined, axis=1), "tp")
    return (combined * lax.rsqrt(out_squares / D + EPS)[:, None] * out_gain).astype(jnp.bfloat16)


def solution(mesh):
    placed = (
        P("ep", "tp"),
        P("tp"),
        P("tp"),
        P(),
        P(),
        P("ep", "tp", None),
        P("ep", "tp", None),
        P("ep", None, "tp"),
    )
    body = on_device
    if mesh.shape["tp"] == 4 and mesh.shape["ep"] == 8:
        body = functools.partial(fused, mesh)
    return jax.shard_map(
        body, mesh=mesh, in_specs=placed, out_specs=P("ep", "tp"), check_vma=False
    )
```
